32 devices in a mesh: sp: 8 (over z, y), tp: 4 (over x, core).
Axes of the slice: x: 2, y: 2, z: 4, core: 2. Of those that a mesh axis runs over, the one named last changes fastest.
Arguments:
- inputs: bfloat16 [4096, 2048], P('sp', 'tp'), may hold values from -6 to 6
- norm_gain: float32 [2048], replicated, may hold values from 0.1 to 1.9
- latent_query: bfloat16 [2048, 1536], P(None, 'tp'), may hold values from -2 to 2
- latent_down: bfloat16 [2048, 512], replicated, may hold values from -2 to 2
- rope_down: bfloat16 [2048, 32], replicated, may hold values from -2 to 2
- latent_gain: float32 [512], replicated, may hold values from 0.1 to 1.9
- latent_up: bfloat16 [512, 2048], P(None, 'tp'), may hold values from -2 to 2
- window_query: bfloat16 [2048, 1024], P(None, 'tp'), may hold values from -2 to 2
- window_key: bfloat16 [2048, 512], P(None, 'tp'), may hold values from -2 to 2
- window_value: bfloat16 [2048, 512], P(None, 'tp'), may hold values from -0.125 to 0.125
- sink_logit: float32 [16], P('tp'), may hold values from 3 to 8
- out_latent: bfloat16 [1024, 2048], P('tp'), may hold values from -0.1875 to 0.1875
- out_window: bfloat16 [1024, 2048], P('tp'), may hold values from -0.1875 to 0.1875
Outputs:
- attended: bfloat16 [4096, 2048], P('sp', 'tp')
The draws below stay inside these ranges and needn't reach their ends.
All inputs are finite; a program needn't handle non-finite values.
Results may differ from the reference program's by a relative error of at most 0.017.
Values may be sent and summed in bfloat16 or wider, within the bound.
A program may use at most 128 MiB of HBM per device.

```python
import jax
import jax.numpy as jnp
from jax import lax

D = 2048
HM = 16
HS = 16
HK = 8
LATENT = 512
NOPE = 64
ROPE = 32
HEAD = 64
WINDOW = 128
TOKENS = 4096
N_TP = 4


def latent_tables(key):
    streams = jax.random.split(jax.random.fold_in(key, 7001), 5)
    lowering = jax.random.normal(streams[0], (D, LATENT), jnp.float32) * D ** (-0.5)
    rotating = jax.random.normal(streams[1], (D, ROPE), jnp.float32) * D ** (-0.5)
    raising = jax.random.normal(streams[2], (LATENT, HM * (NOPE + HEAD)), jnp.float32) * LATENT ** (-0.5)
    queries = jax.random.normal(streams[4], (D, HM * (NOPE + ROPE)), jnp.float32) * 2.5 * D ** (-0.5)
    return (jnp.clip(queries, -2.0, 2.0), jnp.clip(lowering, -2.0, 2.0), jnp.clip(rotating, -2.0, 2.0), jnp.clip(raising, -2.0, 2.0))


def window_tables(key):
    streams = jax.random.split(jax.random.fold_in(key, 7002), 3)
    key_weights = jax.random.normal(streams[0], (D, HK * HEAD), jnp.float32) * D ** (-0.5)
    queries = jax.random.normal(streams[2], (D, HS * HEAD), jnp.float32) * 2.0 * D ** (-0.5)
    return (jnp.clip(queries, -2.0, 2.0), jnp.clip(key_weights, -2.0, 2.0))


def draw_latent_query(key, part):
    return latent_tables(key)[0].astype(jnp.bfloat16)


def draw_latent_down(key, part):
    return latent_tables(key)[1].astype(jnp.bfloat16)


def draw_rope_down(key, part):
    return latent_tables(key)[2].astype(jnp.bfloat16)


def draw_latent_up(key, part):
    return latent_tables(key)[3].astype(jnp.bfloat16)


def draw_window_query(key, part):
    return window_tables(key)[0].astype(jnp.bfloat16)


def draw_window_key(key, part):
    return window_tables(key)[1].astype(jnp.bfloat16)


def level_of(key, dims, pieces, smallest, top_value):
    def one(dim, blocks):
        steps = jax.random.uniform(jax.random.fold_in(jax.random.fold_in(key, 6), dim), (blocks,), jnp.float32, smallest / len(pieces), top_value / len(pieces))
        return jnp.repeat(jnp.exp(steps), dims[dim] // blocks).reshape((-1,) + (1,) * (len(dims) - dim - 1))

    level = one(*pieces[0])
    for cut in pieces[1:]:
        level = level * one(*cut)
    return level


def centred(stream_key, dims, width, most, cuts=(), kind=jnp.bfloat16):
    values = jax.random.normal(stream_key, dims, jnp.float32) * width
    if len(cuts) > 0:
        values = level_of(stream_key, dims, cuts, -0.22, 0.18) * values
    return jnp.clip(values, min=-most, max=most).astype(kind)


def setup_inputs(seed: int = 0) -> dict:
    splits = jax.random.split(jax.random.key(seed), 14)
    return {
        "inputs": centred(splits[0], (TOKENS, D), 1.0, 6.0, ((0, 8), (1, 4))),
        "norm_gain": jnp.clip(1.0 + 0.18 * jax.random.normal(splits[1], (D,), jnp.float32), 0.1, 1.9),
        "latent_query": draw_latent_query(jax.random.fold_in(splits[13], 71), 0),
        "latent_down": draw_latent_down(jax.random.fold_in(splits[13], 71), 0),
        "rope_down": draw_rope_down(jax.random.fold_in(splits[13], 71), 0),
        "latent_gain": jnp.clip(1.0 + 0.18 * jax.random.normal(splits[5], (LATENT,), jnp.float32), 0.1, 1.9),
        "latent_up": draw_latent_up(jax.random.fold_in(splits[13], 71), 0),
        "window_query": draw_window_query(jax.random.fold_in(splits[13], 71), 0),
        "window_key": draw_window_key(jax.random.fold_in(splits[13], 71), 0),
        "window_value": centred(splits[9], (D, HK * HEAD), D ** -0.5, 0.125, ((1, 4),)),
        "sink_logit": jnp.clip(3.0 + 5.0 * jax.random.uniform(splits[10], (HS,), jnp.float32) ** level_of(splits[10], (HS,), ((0, 4),), -0.2, 0.2), 3.0, 8.0),
        "out_latent": centred(splits[11], (HM * HEAD, D), (HM * HEAD) ** -0.5, 0.1875, ((0, 4),)),
        "out_window": centred(splits[12], (HS * HEAD, D), (HS * HEAD) ** -0.5, 0.1875, ((0, 4),)),
    }


epsilon = 1e-06

def rms_scale(values, gains):
    return values * lax.rsqrt(lax.optimization_barrier(jnp.mean(values * values, axis=-1, keepdims=True)) + epsilon) * gains

def rotary(values, positions):
    half_width = values.shape[-1] // 2
    inverse = 1.0 / 10000.0 ** (jnp.arange(0, 2 * half_width, 2).astype(jnp.float32) / (2 * half_width))
    angles = positions[:, None] * inverse[None, :]
    cosine_table = jnp.cos(angles)[:, None, :]
    sine_table = jnp.sin(angles)[:, None, :]
    first_half = values[..., :half_width]
    second_half = values[..., half_width:]
    return jnp.concatenate([first_half * cosine_table - second_half * sine_table, second_half * cosine_table + first_half * sine_table], axis=-1)

def reference(inputs, norm_gain, latent_query, latent_down, rope_down, latent_gain, latent_up, window_query, window_key, window_value, sink_logit, out_latent, out_window):
    length_all = inputs.shape[0]
    positions = jnp.arange(length_all).astype(jnp.float32)
    hidden = rms_scale(inputs.astype(jnp.float32), norm_gain).astype(jnp.bfloat16)
    latent = rms_scale(jnp.dot(hidden, latent_down, preferred_element_type=jnp.float32), latent_gain).astype(jnp.bfloat16)
    shared = rotary(jnp.dot(hidden, rope_down, preferred_element_type=jnp.float32)[:, None, :], positions)[:, 0, :].astype(jnp.bfloat16)
    expanded = jnp.dot(latent, latent_up, preferred_element_type=jnp.float32).astype(jnp.bfloat16)
    expanded = expanded.reshape(length_all, HM, NOPE + HEAD)
    queries = jnp.dot(hidden, latent_query, preferred_element_type=jnp.float32).reshape(length_all, HM, NOPE + ROPE)
    queries = jnp.concatenate([queries[..., :NOPE], rotary(queries[..., NOPE:], positions)], axis=-1).astype(jnp.bfloat16)
    key_plain = expanded[..., :NOPE].astype(jnp.float32)
    value_rows = expanded[..., NOPE:].astype(jnp.float32)
    shared_rows = shared.astype(jnp.float32)
    score_scale = (NOPE + ROPE) ** (-0.5)

    def latent_block(query_block):
        query_block = query_block.astype(jnp.float32)
        scores = (jnp.einsum('qhn,khn->hqk', query_block[..., :NOPE], key_plain) + jnp.einsum('qhr,kr->hqk', query_block[..., NOPE:], shared_rows)) * score_scale
        highest = lax.optimization_barrier(jnp.max(scores, axis=-1, keepdims=True))
        weights = jnp.exp(scores - highest)
        summed = lax.optimization_barrier(jnp.sum(weights, axis=-1))
        rounded = lax.optimization_barrier(weights.astype(jnp.bfloat16)).astype(jnp.float32)
        mixture = jnp.einsum('hqk,khd->qhd', rounded, value_rows)
        return mixture / jnp.transpose(summed)[:, :, None]
    query_blocks = queries.reshape(length_all // WINDOW, WINDOW, HM, NOPE + ROPE)
    latent_out = lax.map(latent_block, query_blocks).reshape(length_all, HM * HEAD).astype(jnp.bfloat16)
    group_size = HS // HK
    block_count = length_all // WINDOW
    window_queries = rotary(jnp.dot(hidden, window_query, preferred_element_type=jnp.float32).reshape(length_all, HS, HEAD), positions).astype(jnp.bfloat16)
    window_keys = rotary(jnp.dot(hidden, window_key, preferred_element_type=jnp.float32).reshape(length_all, HK, HEAD), positions).astype(jnp.bfloat16)
    window_values = jnp.dot(hidden, window_value, preferred_element_type=jnp.float32).astype(jnp.bfloat16).reshape(length_all, HK, HEAD)

    def banded(values):
        padded = jnp.pad(values, ((WINDOW, WINDOW), (0, 0), (0, 0)))
        grid_rows = padded.reshape(block_count + 2, WINDOW, HK, HEAD)
        return jnp.concatenate([grid_rows[:-2], grid_rows[1:-1], grid_rows[2:]], axis=1)
    band_keys = banded(window_keys).astype(jnp.float32)
    band_values = banded(window_values).astype(jnp.float32)
    query_band = window_queries.reshape(block_count, WINDOW, HK, group_size, HEAD).astype(jnp.float32)
    offsets = jnp.arange(3 * WINDOW)[None, :] - jnp.arange(WINDOW)[:, None]
    key_pos = jnp.arange(block_count)[:, None] * WINDOW - WINDOW + jnp.arange(3 * WINDOW)[None, :]
    allowed = ((offsets >= 0) & (offsets <= 2 * WINDOW))[None] & ((key_pos >= 0) & (key_pos < length_all))[:, None, :]
    sink_table = sink_logit.reshape(HK, group_size)

    def window_head(operands):
        head_queries, head_keys, head_values, head_sinks = operands
        scores = jnp.einsum('nqgd,nkd->ngqk', head_queries, head_keys) * HEAD ** (-0.5)
        scores = jnp.where(allowed[:, None], scores, -jnp.inf)
        highest = jnp.maximum(lax.optimization_barrier(jnp.max(scores, axis=-1)), head_sinks[None, :, None])
        weights = jnp.exp(scores - highest[..., None])
        summed = lax.optimization_barrier(jnp.sum(weights, axis=-1)) + jnp.exp(head_sinks[None, :, None] - highest)
        rounded = lax.optimization_barrier(weights.astype(jnp.bfloat16)).astype(jnp.float32)
        mixture = jnp.einsum('ngqk,nkd->nqgd', rounded, head_values)
        return mixture / jnp.transpose(summed, (0, 2, 1))[..., None]
    stacked = lax.map(window_head, (jnp.moveaxis(query_band, 2, 0), jnp.moveaxis(band_keys, 2, 0), jnp.moveaxis(band_values, 2, 0), sink_table))
    window_out = jnp.moveaxis(stacked, 0, 2).reshape(length_all, HS * HEAD).astype(jnp.bfloat16)
    latent_cols = HM * HEAD // N_TP
    window_cols = HS * HEAD // N_TP
    result = jnp.zeros((length_all, D), jnp.float32)
    for group_index in range(N_TP):
        partial_value = jnp.dot(latent_out[:, group_index * latent_cols:(group_index + 1) * latent_cols], out_latent[group_index * latent_cols:(group_index + 1) * latent_cols], preferred_element_type=jnp.float32)
        partial_value = partial_value + jnp.dot(window_out[:, group_index * window_cols:(group_index + 1) * window_cols], out_window[group_index * window_cols:(group_index + 1) * window_cols], preferred_element_type=jnp.float32)
        result = result + lax.optimization_barrier(partial_value.astype(jnp.bfloat16)).astype(jnp.float32)
    return result.astype(jnp.bfloat16)
```

```python
import functools
import math

import jax
import jax.numpy as jnp
import numpy as np
from jax import lax
from jax.experimental import pallas as pl
from jax.experimental.pallas import tpu as pltpu
from jax.sharding import PartitionSpec as P

NOPE = 64
ROPE = 32
HEAD = 64
WINDOW = 128
EPS = 1e-06
LOG2E = math.log2(math.e)
F32 = jnp.float32
BF16 = jnp.bfloat16
CH = 128


def ring_tables(count):
    bits = count.bit_length() - 1
    ny = 2 ** (bits // 2)
    nz = count // ny
    order = [z * ny for z in range(nz)]
    for step, z in enumerate(reversed(range(nz))):
        row = [z * ny + y for y in range(1, ny)]
        order += row if step % 2 == 0 else row[::-1]
    return ny, nz, order


def cycle_position(s, ny, nz):
    z, y = s // ny, s % ny
    step = nz - 1 - z
    even = step % 2 == 0
    inner = jnp.where(even, y - 1, ny - 1 - y)
    return jnp.where(y == 0, z, nz + step * (ny - 1) + inner)


def cycle_member(p, ny, nz):
    q = jnp.maximum(p - nz, 0)
    step = q // (ny - 1)
    inner = q % (ny - 1)
    y = jnp.where(step % 2 == 0, inner + 1, ny - 1 - inner)
    return jnp.where(p < nz, p * ny, (nz - 1 - step) * ny + y)


def rotate(v, cos, sin):
    half = v.shape[-1] // 2
    a, b = v[:, :half], v[:, half:]
    return jnp.concatenate([a * cos - b * sin, b * cos + a * sin], axis=-1)


def body(dims, *refs):
    (n_sp, n_tp, rows, feat, heads, wheads, kheads) = dims
    (x_ref, gain_ref, lq_h, ld_h, rd_h, lgain_ref, lu_h, wq_h, wk_h, wv_h, sink_ref,
     ol_h, ow_h, cp_ref, cq_ref, off_ref, out_ref,
     lq, ld, rd, lu, wq, wk, wv, ol, ow, xg, hid, lat, krt, qs, qw, wkb, wvb,
     kop, vop, acc, mx, oml, omw, part_p, part_m, prec, xs, xr,
     wsem, xsend, xrecv, xfsend, lsend, lrecv, lfsend, ksend, krecv, kfsend,
     hsend, hrecv, psend, precv, ssend, srecv) = refs
    nr = rows // CH
    nx = n_tp // 2
    group = wheads // kheads
    sp = lax.axis_index("sp")
    tp = lax.axis_index("tp")
    xi, core = tp // 2, tp % 2
    mate = xi * 2 + (1 - core)
    ny, nz, _ = ring_tables(n_sp)
    pos = cycle_position(sp, ny, nz)

    def member(delta):
        return cycle_member(lax.rem(pos + delta + n_sp, n_sp), ny, nz)

    right, left = member(1), member(-1)
    above, below = lax.rem(sp + 1, n_sp), lax.rem(sp + n_sp - 1, n_sp)

    def at(s=None, t=None):
        return {"sp": sp if s is None else s, "tp": tp if t is None else t}

    def rcopy(src, dst, ss, rs, dev):
        return pltpu.make_async_remote_copy(
            src_ref=src, dst_ref=dst, send_sem=ss, recv_sem=rs,
            device_id=dev, device_id_type=pl.DeviceIdType.MESH)

    weights = [pltpu.make_async_copy(h, v, wsem.at[i]) for i, (h, v) in enumerate(
        [(ld_h, ld), (rd_h, rd), (lq_h, lq), (wq_h, wq), (wk_h, wk), (wv_h, wv),
         (lu_h, lu), (ol_h, ol), (ow_h, ow)])]
    for w in weights:
        w.start()

    def xpeer(dx):
        return lax.rem(xi + dx, nx)

    barrier = pltpu.get_barrier_semaphore()
    peers = [at(t=xpeer(dx) * 2 + core) for dx in range(1, nx)]
    peers += [at(t=mate), at(s=right), at(s=left), at(s=above), at(s=below)]
    for dev in peers:
        pl.semaphore_signal(barrier, inc=1, device_id=dev, device_id_type=pl.DeviceIdType.MESH)
    pl.semaphore_wait(barrier, len(peers))

    def xsrc(r):
        return x_ref.at[pl.ds(pl.multiple_of(r * CH, CH), CH)]

    def xcopy(r, dx):
        return rcopy(xsrc(r), xg.at[tp, r], xsend.at[dx, r], xrecv.at[tp, r],
                     at(t=xpeer(dx) * 2 + core))

    def xmate(r):
        return rcopy(xsrc(r), xg.at[tp, r], xsend.at[0, r], xrecv.at[tp, r], at(t=mate))

    def xforward(r, dx):
        src = xpeer(dx) * 2 + core
        return rcopy(xg.at[src, r], xg.at[src, r], xfsend.at[dx, r], xrecv.at[src, r], at(t=mate))

    def xwait(src, r):
        rcopy(xg.at[src, r], xg.at[src, r], xsend.at[0, r], xrecv.at[src, r],
              at(t=mate)).wait_recv()

    def start_x(r, _):
        for dx in range(1, nx):
            xcopy(r, dx).start()
        xmate(r).start()
        return 0

    lax.fori_loop(0, nr, start_x, 0)
    for w in weights[:6]:
        w.wait()

    def uslot(b, r):
        return lat.at[b, r], krt.at[b, r]

    def ring_copies(b, r, way, dev):
        j = r // 2
        l, k = uslot(b, r)
        return [rcopy(l, l, lsend.at[way, b, j], lrecv.at[b, r], dev),
                rcopy(k, k, ksend.at[way, b, j], krecv.at[b, r], dev)]

    def mate_copies(b, r):
        j = r // 2
        l, k = uslot(b, r)
        return [rcopy(l, l, lfsend.at[b, j], lrecv.at[b, r], at(t=mate)),
                rcopy(k, k, kfsend.at[b, j], krecv.at[b, r], at(t=mate))]

    def halo(i):
        src = 1 if i == 0 else nr
        dst = nr + 1 if i == 0 else 0
        dev = at(s=below) if i == 0 else at(s=above)
        return [rcopy(wkb.at[src], wkb.at[dst], hsend.at[i, 0], hrecv.at[i, 0], dev),
                rcopy(wvb.at[src], wvb.at[dst], hsend.at[i, 1], hrecv.at[i, 1], dev)]

    def project(r):
        span = pl.ds(pl.multiple_of(r * CH, CH), CH)
        ssq = jnp.zeros((CH, 1), F32)
        for t in range(n_tp):
            xf = xg[t, r].astype(F32)
            ssq = ssq + jnp.sum(xf * xf, axis=-1, keepdims=True)
            hid[:, t * feat:(t + 1) * feat] = (
                xf * gain_ref[:, t * feat:(t + 1) * feat]).astype(BF16)
        scale = lax.rsqrt(ssq / (n_tp * feat) + EPS)
        tab = cp_ref[span, :] * off_ref[sp, 0:1, :] + cq_ref[span, :] * off_ref[sp, 1:2, :]
        cos_w, sin_w = tab[:, 0:32], tab[:, 32:64]
        cos_l, sin_l = tab[:, 64:80], tab[:, 80:96]
        low = jnp.dot(hid[...], ld[...], preferred_element_type=F32) * scale
        low = low * lax.rsqrt(jnp.mean(low * low, axis=-1, keepdims=True) + EPS) * lgain_ref[...]
        lat[sp, r] = low.astype(BF16)
        shared = jnp.dot(hid[...], rd[...], preferred_element_type=F32) * scale
        shared = rotate(shared, cos_l, sin_l)
        wide = jnp.concatenate([shared, jnp.zeros((CH, CH - ROPE), F32)], axis=-1)
        krt[sp, r] = wide.T[:ROPE].astype(BF16)

        @pl.when(r % 2 == core)
        def _():
            for c in ring_copies(sp, r, 0, at(s=right)) + ring_copies(sp, r, 1, at(s=left)):
                c.start()

        keys = jnp.dot(hid[...], wk[...], preferred_element_type=F32) * scale
        keys = jnp.concatenate(
            [rotate(keys[:, g * HEAD:(g + 1) * HEAD], cos_w, sin_w) for g in range(kheads)], axis=-1)
        wkb[r + 1] = keys.astype(BF16)
        wvb[r + 1] = (jnp.dot(hid[...], wv[...], preferred_element_type=F32) * scale).astype(BF16)

        @pl.when(r == 0)
        def _():
            for c in halo(0):
                c.start()

        @pl.when(r == nr - 1)
        def _():
            for c in halo(1):
                c.start()

        q = jnp.dot(hid[...], lq[...], preferred_element_type=F32) * (
            scale * ((NOPE + ROPE) ** -0.5 * LOG2E))
        width = NOPE + ROPE
        for h in range(heads):
            qh = q[:, h * width:(h + 1) * width]
            qs[h, span, :] = jnp.concatenate(
                [qh[:, :NOPE], rotate(qh[:, NOPE:], cos_l, sin_l),
                 jnp.zeros((CH, 128 - width), F32)], axis=-1).astype(BF16)
        q = jnp.dot(hid[...], wq[...], preferred_element_type=F32) * (
            scale * (HEAD ** -0.5 * LOG2E))
        for g in range(wheads):
            qh = rotate(q[:, g * HEAD:(g + 1) * HEAD], cos_w, sin_w)
            kv = g // group
            pieces = [qh if i == kv else jnp.zeros_like(qh) for i in range(kheads)]
            qw[g, span, :] = jnp.concatenate(pieces, axis=-1).astype(BF16)

    def gather_step(e, _):
        @pl.when(e < nr)
        def _():
            r = e
            xg[tp, r] = x_ref[pl.ds(pl.multiple_of(r * CH, CH), CH), :]
            for dx in range(1, nx):
                xwait(xpeer(dx) * 2 + core, r)
                xforward(r, dx).start()

        @pl.when(e >= 1)
        def _():
            r = e - 1
            for dx in range(nx):
                xwait(xpeer(dx) * 2 + 1 - core, r)
            project(r)
        return 0

    lax.fori_loop(0, nr + 1, gather_step, 0)
    weights[6].wait()

    acc[...] = jnp.zeros_like(acc)
    mx[...] = jnp.full_like(mx, -1e30)
    lane = lax.broadcasted_iota(jnp.int32, (CH, CH), 1)

    def block(b):
        def expand(r, _):
            e = jnp.dot(lat[b, r], lu[...], preferred_element_type=F32)
            kt = jnp.concatenate(
                [jnp.zeros((NOPE, CH), F32), krt[b, r].astype(F32),
                 jnp.zeros((128 - NOPE - ROPE, CH), F32)], axis=0).T
            span = pl.ds(pl.multiple_of(r * CH, CH), CH)
            for h in range(heads):
                eh = e[:, h * 128:(h + 1) * 128]
                kop[h, span, :] = jnp.where(lane < NOPE, eh, kt).astype(BF16)
                vop[h, span, :] = jnp.where(lane < NOPE, 1.0, eh).astype(BF16)
            return 0

        lax.fori_loop(0, nr, expand, 0)
        qt = 256
        tiles = rows // qt

        def tile(i, _):
            h, t = i // tiles, i % tiles
            span = pl.ds(pl.multiple_of(t * qt, qt), qt)
            s = lax.dot_general(qs[h, span, :], kop[h], (((1,), (1,)), ((), ())),
                                preferred_element_type=F32)
            old = mx[h, span, :]
            new = jnp.maximum(old, jnp.max(s, axis=-1, keepdims=True))
            p = jnp.exp2(s - new[:, 0:1]).astype(BF16)
            acc[h, span, :] = acc[h, span, :] * jnp.exp2(old - new) + jnp.dot(
                p, vop[h], preferred_element_type=F32)
            mx[h, span, :] = new
            return 0

        lax.fori_loop(0, heads * tiles, tile, 0)

    def window():
        for i in range(2):
            for c in halo(i):
                c.wait_recv()

        def one(n, _):
            kk = wkb[pl.ds(n, 3)].reshape(3 * CH, wkb.shape[-1])
            vv = wvb[pl.ds(n, 3)].reshape(3 * CH, wvb.shape[-1])
            qi = lax.broadcasted_iota(jnp.int32, (CH, 3 * CH), 0)
            ki = lax.broadcasted_iota(jnp.int32, (CH, 3 * CH), 1)
            kp = sp * rows + (n - 1) * CH + ki
            ok = (ki - qi >= 0) & (ki - qi <= 2 * WINDOW) & (kp >= 0) & (kp < n_sp * rows)
            span = pl.ds(pl.multiple_of(n * CH, CH), CH)
            outs = []
            for g in range(wheads):
                kv = g // group
                s = lax.dot_general(qw[g, span, :], kk, (((1,), (1,)), ((), ())),
                                    preferred_element_type=F32)
                s = jnp.where(ok, s, -1e30)
                sink = sink_ref[0:1, g:g + 1] * LOG2E
                m = jnp.maximum(jnp.max(s, axis=-1, keepdims=True), sink)
                p = jnp.exp2(s - m)
                den = jnp.sum(p, axis=-1, keepdims=True) + jnp.exp2(sink - m)
                o = jnp.dot(p.astype(BF16), vv, preferred_element_type=F32) / den
                outs.append(o[:, kv * HEAD:(kv + 1) * HEAD])
            omw[span, :] = jnp.concatenate(outs, axis=-1).astype(BF16)
            return 0

        lax.fori_loop(0, nr, one, 0)

    half = n_sp // 2

    def ring_step(e, _):
        d, j = e // 2 + 1, e % 2
        r = 2 * j + core
        for way in range(2):
            last = half - core if way == 0 else half - 1 + core
            b = member(-d) if way == 0 else member(d)
            dev = at(s=right) if way == 0 else at(s=left)

            @pl.when((e < n_sp) & (d <= last))
            def _():
                for c in ring_copies(b, r, way, dev):
                    c.wait_recv()

                @pl.when(d < last)
                def _():
                    for c in ring_copies(b, r, way, dev):
                        c.start()

                for c in mate_copies(b, r):
                    c.start()

        d1 = e // 2
        b = jnp.where(e == 0, sp, jnp.where(j == 0, member(-d1), member(d1)))

        @pl.when(e >= 2)
        def _():
            for i in range(nr // 2):
                for c in mate_copies(b, 2 * i + 1 - core):
                    c.wait_recv()

        @pl.when(e == 1)
        def _():
            window()

        @pl.when(e != 1)
        def _():
            block(b)
        return 0

    lax.fori_loop(0, n_sp + 1, ring_step, 0)
    weights[7].wait()
    weights[8].wait()

    for i in range(heads // 2):
        def norm(h):
            a = acc[h]
            return a, pltpu.roll(a, NOPE, 1)
        a0, b0 = norm(2 * i)
        a1, b1 = norm(2 * i + 1)
        low = lax.broadcasted_iota(jnp.int32, a0.shape, 1) < NOPE
        oml[:, i * 128:(i + 1) * 128] = (
            jnp.where(low, b0, a1) / jnp.where(low, a0, b1)).astype(BF16)

    def pcopy(r, k):
        return rcopy(part_p.at[k, r], prec.at[k, r], psend.at[k, r], precv.at[k, r], at(t=mate))

    def scopy(r, dx):
        k = xpeer(dx)
        return rcopy(xs.at[dx, r], xr.at[dx, r], ssend.at[dx, r], srecv.at[dx, r],
                     at(t=k * 2 + core))

    def partial(r, t):
        span = pl.ds(pl.multiple_of(r * CH, CH), CH)
        cols = pl.ds(pl.multiple_of(t * feat, 128), feat)
        return jnp.dot(oml[span, :], ol[:, cols], preferred_element_type=F32) + jnp.dot(
            omw[span, :], ow[:, cols], preferred_element_type=F32)

    def scatter_step(e, _):
        @pl.when(e < nr)
        def _():
            for k in range(nx):
                part_p[k, e] = partial(e, 2 * k + 1 - core).astype(BF16)
                pcopy(e, k).start()
            for k in range(nx):
                part_m[k, e] = partial(e, 2 * k + core)

        @pl.when(e >= 1)
        def _():
            r = e - 1
            for k in range(nx):
                pcopy(r, k).wait_recv()
            for dx in range(1, nx):
                k = xpeer(dx)
                xs[dx, r] = (part_m[k, r] + prec[k, r].astype(F32)).astype(BF16)
                scopy(r, dx).start()
        return 0

    lax.fori_loop(0, nr + 1, scatter_step, 0)

    def final_step(r, _):
        total = part_m[xi, r] + prec[xi, r].astype(F32)
        for dx in range(1, nx):
            scopy(r, dx).wait_recv()
            total = total + xr[dx, r].astype(F32)
        out_ref[pl.ds(pl.multiple_of(r * CH, CH), CH), :] = total.astype(BF16)
        return 0

    lax.fori_loop(0, nr, final_step, 0)

    def drain_rows(r, _):
        xmate(r).wait_send()
        for dx in range(1, nx):
            xcopy(r, dx).wait_send()
            xforward(r, dx).wait_send()
            scopy(r, dx).wait_send()
        for k in range(nx):
            pcopy(r, k).wait_send()
        return 0

    lax.fori_loop(0, nr, drain_rows, 0)
    for i in range(2):
        for c in halo(i):
            c.wait_send()

    def drain_ring(e, _):
        d, j = e // 2, e % 2
        r = 2 * j + core
        for way in range(2):
            last = half - core if way == 0 else half - 1 + core
            b = member(-d) if way == 0 else member(d)
            dev = at(s=right) if way == 0 else at(s=left)

            @pl.when(d < last)
            def _():
                for c in ring_copies(b, r, way, dev):
                    c.wait_send()

            @pl.when((d >= 1) & (d <= last))
            def _():
                for c in mate_copies(b, r):
                    c.wait_send()
        return 0

    lax.fori_loop(0, n_sp + 2, drain_ring, 0)


def tables(rows, n_sp):
    freq_w = 10000.0 ** (-np.arange(32) / 32.0)
    freq_l = 10000.0 ** (-np.arange(16) / 16.0)
    freq = np.concatenate([freq_w, freq_w, freq_l, freq_l, np.zeros(32)])
    is_sin = np.concatenate(
        [np.zeros(32), np.ones(32), np.zeros(16), np.ones(16), np.zeros(32)]) > 0
    inner = np.arange(rows)[:, None] * freq[None]
    c, s = np.cos(inner), np.sin(inner)
    first = np.where(is_sin, s, c).astype(np.float32)
    second = np.where(is_sin, c, -s).astype(np.float32)
    outer = (np.arange(n_sp) * rows)[:, None] * freq[None]
    offs = np.stack([np.cos(outer), np.sin(outer)], axis=1).astype(np.float32)
    return first, second, offs


def shards(n_sp, n_tp, x, gain, lq, ld, rd, lgain, lu, wq, wk, wv, sink, ol, ow):
    rows, feat = x.shape
    nr = rows // CH
    nx = n_tp // 2
    heads = lu.shape[1] // (NOPE + HEAD)
    wheads = wq.shape[1] // HEAD
    kheads = wk.shape[1] // HEAD
    latent = ld.shape[1]
    dims = (n_sp, n_tp, rows, feat, heads, wheads, kheads)
    first, second, offs = tables(rows, n_sp)
    vm = pl.BlockSpec(memory_space=pltpu.VMEM)
    hb = pl.BlockSpec(memory_space=pl.ANY)
    big = [lq, ld, rd, lu, wq, wk, wv, ol, ow]
    dma = pltpu.SemaphoreType.DMA
    scratch = [pltpu.VMEM(a.shape, a.dtype) for a in big] + [
        pltpu.VMEM((n_tp, nr, CH, feat), BF16),
        pltpu.VMEM((CH, n_tp * feat), BF16),
        pltpu.VMEM((n_sp, nr, CH, latent), BF16),
        pltpu.VMEM((n_sp, nr, ROPE, CH), BF16),
        pltpu.VMEM((heads, rows, 128), BF16),
        pltpu.VMEM((wheads, rows, kheads * HEAD), BF16),
        pltpu.VMEM((nr + 2, CH, kheads * HEAD), BF16),
        pltpu.VMEM((nr + 2, CH, kheads * HEAD), BF16),
        pltpu.VMEM((heads, rows, 128), BF16),
        pltpu.VMEM((heads, rows, 128), BF16),
        pltpu.VMEM((heads, rows, 128), F32),
        pltpu.VMEM((heads, rows, 128), F32),
        pltpu.VMEM((rows, heads * HEAD), BF16),
        pltpu.VMEM((rows, wheads * HEAD), BF16),
        pltpu.VMEM((nx, nr, CH, feat), BF16),
        pltpu.VMEM((nx, nr, CH, feat), F32),
        pltpu.VMEM((nx, nr, CH, feat), BF16),
        pltpu.VMEM((nx, nr, CH, feat), BF16),
        pltpu.VMEM((nx, nr, CH, feat), BF16),
        dma((9,)),
        dma((nx, nr)), dma((n_tp, nr)), dma((nx, nr)),
        dma((2, n_sp, 2)), dma((n_sp, nr)), dma((n_sp, 2)),
        dma((2, n_sp, 2)), dma((n_sp, nr)), dma((n_sp, 2)),
        dma((2, 2)), dma((2, 2)),
        dma((nx, nr)), dma((nx, nr)), dma((nx, nr)), dma((nx, nr)),
    ]
    return pl.pallas_call(
        functools.partial(body, dims),
        out_shape=jax.ShapeDtypeStruct((rows, feat), BF16),
        in_specs=[vm, vm, hb, hb, hb, vm, hb, hb, hb, hb, vm, hb, hb, vm, vm, vm],
        out_specs=vm,
        scratch_shapes=scratch,
        compiler_params=pltpu.CompilerParams(
            collective_id=0, has_side_effects=True, vmem_limit_bytes=60 * 1024 * 1024),
    )(x, gain[None], lq, ld, rd, lgain[None], lu, wq, wk, wv, sink[None], ol, ow,
      jnp.asarray(first), jnp.asarray(second), jnp.asarray(offs))


def solution(mesh):
    in_specs = (
        P("sp", "tp"),
        P(),
        P(None, "tp"),
        P(),
        P(),
        P(),
        P(None, "tp"),
        P(None, "tp"),
        P(None, "tp"),
        P(None, "tp"),
        P("tp"),
        P("tp", None),
        P("tp", None),
    )
    step = functools.partial(shards, mesh.shape["sp"], mesh.shape["tp"])
    return jax.shard_map(
        step, mesh=mesh, in_specs=in_specs, out_specs=P("sp", "tp"), check_vma=False)
```

```python
import functools
import math

import jax
import jax.numpy as jnp
import numpy as np
from jax import lax
from jax.experimental import pallas as pl
from jax.experimental.pallas import tpu as pltpu
from jax.sharding import PartitionSpec as P

NOPE = 64
ROPE = 32
HEAD = 64
WINDOW = 128
EPS = 1e-06
LOG2E = math.log2(math.e)
F32 = jnp.float32
BF16 = jnp.bfloat16
CH = 128


def ring_tables(count):
    bits = count.bit_length() - 1
    ny = 2 ** (bits // 2)
    nz = count // ny
    order = [z * ny for z in range(nz)]
    for step, z in enumerate(reversed(range(nz))):
        row = [z * ny + y for y in range(1, ny)]
        order += row if step % 2 == 0 else row[::-1]
    return ny, nz, order


def cycle_position(s, ny, nz):
    z, y = s // ny, s % ny
    step = nz - 1 - z
    even = step % 2 == 0
    inner = jnp.where(even, y - 1, ny - 1 - y)
    return jnp.where(y == 0, z, nz + step * (ny - 1) + inner)


def cycle_member(p, ny, nz):
    q = jnp.maximum(p - nz, 0)
    step = q // (ny - 1)
    inner = q % (ny - 1)
    y = jnp.where(step % 2 == 0, inner + 1, ny - 1 - inner)
    return jnp.where(p < nz, p * ny, (nz - 1 - step) * ny + y)


def rotate(v, cos, sin):
    half = v.shape[-1] // 2
    a, b = v[:, :half], v[:, half:]
    return jnp.concatenate([a * cos - b * sin, b * cos + a * sin], axis=-1)


def body(dims, *refs):
    (n_sp, n_tp, rows, feat, heads, wheads, kheads) = dims
    (x_ref, gain_ref, lq_h, ld_h, rd_h, lgain_ref, lu_h, wq_h, wk_h, wv_h, sink_ref,
     ol_h, ow_h, cp_ref, cq_ref, off_ref, out_ref,
     lq, ld, rd, lu, wq, wk, wv, ol, ow, xg, hid, lat, krt, qs, qw, wkb, wvb,
     luk, kop, vop, acc, mx, oml, omw, part_p, part_m, prec, xs, xr,
     wsem, xsend, xrecv, xfsend, lsend, lrecv, lfsend, ksend, krecv, kfsend,
     hsend, hrecv, psend, precv, ssend, srecv) = refs
    nr = rows // CH
    nx = n_tp // 2
    group = wheads // kheads
    sp = lax.axis_index("sp")
    tp = lax.axis_index("tp")
    xi, core = tp // 2, tp % 2
    mate = xi * 2 + (1 - core)
    ny, nz, _ = ring_tables(n_sp)
    pos = cycle_position(sp, ny, nz)

    def member(delta):
        return cycle_member(lax.rem(pos + delta + n_sp, n_sp), ny, nz)

    right, left = member(1), member(-1)
    above, below = lax.rem(sp + 1, n_sp), lax.rem(sp + n_sp - 1, n_sp)

    def at(s=None, t=None):
        return {"sp": sp if s is None else s, "tp": tp if t is None else t}

    def rcopy(src, dst, ss, rs, dev):
        return pltpu.make_async_remote_copy(
            src_ref=src, dst_ref=dst, send_sem=ss, recv_sem=rs,
            device_id=dev, device_id_type=pl.DeviceIdType.MESH)

    weights = [pltpu.make_async_copy(h, v, wsem.at[i]) for i, (h, v) in enumerate(
        [(ld_h, ld), (rd_h, rd), (lq_h, lq), (wq_h, wq), (wk_h, wk), (wv_h, wv),
         (lu_h, lu), (ol_h, ol), (ow_h, ow)])]
    for w in weights:
        w.start()

    def xpeer(dx):
        return lax.rem(xi + dx, nx)

    barrier = pltpu.get_barrier_semaphore()
    peers = [at(t=xpeer(dx) * 2 + core) for dx in range(1, nx)]
    peers += [at(t=mate), at(s=right), at(s=left), at(s=above), at(s=below)]
    for dev in peers:
        pl.semaphore_signal(barrier, inc=1, device_id=dev, device_id_type=pl.DeviceIdType.MESH)
    pl.semaphore_wait(barrier, len(peers))

    def xsrc(r):
        return x_ref.at[pl.ds(pl.multiple_of(r * CH, CH), CH)]

    def xcopy(r, dx):
        return rcopy(xsrc(r), xg.at[tp, r], xsend.at[dx, r], xrecv.at[tp, r],
                     at(t=xpeer(dx) * 2 + core))

    def xmate(r):
        return rcopy(xsrc(r), xg.at[tp, r], xsend.at[0, r], xrecv.at[tp, r], at(t=mate))

    def xforward(r, dx):
        src = xpeer(dx) * 2 + core
        return rcopy(xg.at[src, r], xg.at[src, r], xfsend.at[dx, r], xrecv.at[src, r], at(t=mate))

    def xwait(src, r):
        rcopy(xg.at[src, r], xg.at[src, r], xsend.at[0, r], xrecv.at[src, r],
              at(t=mate)).wait_recv()

    def start_x(r, _):
        for dx in range(1, nx):
            xcopy(r, dx).start()
        xmate(r).start()
        return 0

    lax.fori_loop(0, nr, start_x, 0)
    acc[...] = jnp.zeros_like(acc)
    mx[...] = jnp.full_like(mx, -1e30)
    kop[...] = jnp.zeros_like(kop)
    for w in weights[:7]:
        w.wait()
    for h in range(heads):
        luk[h * NOPE:(h + 1) * NOPE, :] = (
            lu[:, h * 128:(h + 1) * 128].astype(F32).T[:NOPE].astype(BF16))

    def uslot(b, r):
        return lat.at[b, r], krt.at[b, r]

    def ring_copies(b, r, way, dev):
        j = r // 2
        l, k = uslot(b, r)
        return [rcopy(l, l, lsend.at[way, b, j], lrecv.at[b, r], dev),
                rcopy(k, k, ksend.at[way, b, j], krecv.at[b, r], dev)]

    def mate_copies(b, r):
        j = r // 2
        l, k = uslot(b, r)
        return [rcopy(l, l, lfsend.at[b, j], lrecv.at[b, r], at(t=mate)),
                rcopy(k, k, kfsend.at[b, j], krecv.at[b, r], at(t=mate))]

    def halo(i):
        src = 1 if i == 0 else nr
        dst = nr + 1 if i == 0 else 0
        dev = at(s=below) if i == 0 else at(s=above)
        return [rcopy(wkb.at[src], wkb.at[dst], hsend.at[i, 0], hrecv.at[i, 0], dev),
                rcopy(wvb.at[src], wvb.at[dst], hsend.at[i, 1], hrecv.at[i, 1], dev)]

    def project(r):
        span = pl.ds(pl.multiple_of(r * CH, CH), CH)
        ssq = jnp.zeros((CH, 1), F32)
        for t in range(n_tp):
            xf = xg[t, r].astype(F32)
            ssq = ssq + jnp.sum(xf * xf, axis=-1, keepdims=True)
            hid[:, t * feat:(t + 1) * feat] = (
                xf * gain_ref[:, t * feat:(t + 1) * feat]).astype(BF16)
        scale = lax.rsqrt(ssq / (n_tp * feat) + EPS)
        tab = cp_ref[span, :] * off_ref[sp, 0:1, :] + cq_ref[span, :] * off_ref[sp, 1:2, :]
        cos_w, sin_w = tab[:, 0:32], tab[:, 32:64]
        cos_l, sin_l = tab[:, 64:80], tab[:, 80:96]
        low = jnp.dot(hid[...], ld[...], preferred_element_type=F32) * scale
        low = low * lax.rsqrt(jnp.mean(low * low, axis=-1, keepdims=True) + EPS) * lgain_ref[...]
        lat[sp, r] = low.astype(BF16)
        shared = lax.dot_general(hid[...], rd[...], (((1,), (1,)), ((), ())),
                                 preferred_element_type=F32) * scale
        shared = rotate(shared, cos_l, sin_l)
        wide = jnp.concatenate([shared, jnp.zeros((CH, CH - ROPE), F32)], axis=-1)
        krt[sp, r] = wide.T[:ROPE].astype(BF16)

        @pl.when(r % 2 == core)
        def _():
            for c in ring_copies(sp, r, 0, at(s=right)) + ring_copies(sp, r, 1, at(s=left)):
                c.start()

        keys = jnp.dot(hid[...], wk[...], preferred_element_type=F32) * scale
        keys = jnp.concatenate(
            [rotate(keys[:, g * HEAD:(g + 1) * HEAD], cos_w, sin_w) for g in range(kheads)], axis=-1)
        wkb[r + 1] = keys.astype(BF16)
        wvb[r + 1] = (jnp.dot(hid[...], wv[...], preferred_element_type=F32) * scale).astype(BF16)

        @pl.when(r == 0)
        def _():
            for c in halo(0):
                c.start()

        @pl.when(r == nr - 1)
        def _():
            for c in halo(1):
                c.start()

        q = jnp.dot(hid[...], lq[...], preferred_element_type=F32) * (
            scale * ((NOPE + ROPE) ** -0.5 * LOG2E))
        width = NOPE + ROPE
        for h in range(heads):
            qh = q[:, h * width:(h + 1) * width]
            qs[h, span, :] = jnp.concatenate(
                [qh[:, :NOPE], rotate(qh[:, NOPE:], cos_l, sin_l),
                 jnp.zeros((CH, 128 - width), F32)], axis=-1).astype(BF16)
        q = jnp.dot(hid[...], wq[...], preferred_element_type=F32) * (
            scale * (HEAD ** -0.5 * LOG2E))
        for g in range(wheads):
            qh = rotate(q[:, g * HEAD:(g + 1) * HEAD], cos_w, sin_w)
            kv = g // group
            pieces = [qh if i == kv else jnp.zeros_like(qh) for i in range(kheads)]
            qw[g, span, :] = jnp.concatenate(pieces, axis=-1).astype(BF16)

    def gather_step(e, _):
        @pl.when(e < nr)
        def _():
            r = e
            xg[tp, r] = x_ref[pl.ds(pl.multiple_of(r * CH, CH), CH), :]
            for dx in range(1, nx):
                xwait(xpeer(dx) * 2 + core, r)
                xforward(r, dx).start()

        @pl.when(e >= 1)
        def _():
            r = e - 1
            for dx in range(nx):
                xwait(xpeer(dx) * 2 + 1 - core, r)
            project(r)
        return 0

    lax.fori_loop(0, nr + 1, gather_step, 0)
    lane = lax.broadcasted_iota(jnp.int32, (rows, 128), 1)

    def block(b):
        keys = lat[b].reshape(rows, lat.shape[-1])
        et = lax.dot_general(luk[...], keys, (((1,), (1,)), ((), ())),
                             preferred_element_type=F32).astype(BF16)
        ev = jnp.dot(keys, lu[...], preferred_element_type=F32)
        for h in range(heads):
            kop[h, 0:NOPE, :] = et[h * NOPE:(h + 1) * NOPE]
            for r in range(nr):
                kop[h, NOPE:NOPE + ROPE, r * CH:(r + 1) * CH] = krt[b, r]
            vop[h] = jnp.where(lane < NOPE, 1.0, ev[:, h * 128:(h + 1) * 128]).astype(BF16)
        qt = 256
        tiles = rows // qt

        def tile(t, _):
            span = pl.ds(pl.multiple_of(t * qt, qt), qt)

            def score(h):
                return jnp.dot(qs[h, span, :], kop[h], preferred_element_type=F32)

            s = score(0)
            for h in range(heads):
                ahead = score(h + 1) if h + 1 < heads else None
                old = mx[h, span, :]
                new = jnp.maximum(old, jnp.max(s, axis=-1, keepdims=True))
                p = jnp.exp2(s - jnp.concatenate([new] * (rows // 128), axis=-1)).astype(BF16)
                acc[h, span, :] = acc[h, span, :] * jnp.exp2(old - new) + jnp.dot(
                    p, vop[h], preferred_element_type=F32)
                mx[h, span, :] = new
                s = ahead
            return 0

        lax.fori_loop(0, tiles, tile, 0)

    def window():
        for i in range(2):
            for c in halo(i):
                c.wait_recv()

        def one(n, _):
            kk = wkb[pl.ds(n, 3)].reshape(3 * CH, wkb.shape[-1])
            vv = wvb[pl.ds(n, 3)].reshape(3 * CH, wvb.shape[-1])
            qi = lax.broadcasted_iota(jnp.int32, (CH, 3 * CH), 0)
            ki = lax.broadcasted_iota(jnp.int32, (CH, 3 * CH), 1)
            kp = sp * rows + (n - 1) * CH + ki
            ok = (ki - qi >= 0) & (ki - qi <= 2 * WINDOW) & (kp >= 0) & (kp < n_sp * rows)
            span = pl.ds(pl.multiple_of(n * CH, CH), CH)
            outs = []
            for g in range(wheads):
                kv = g // group
                s = lax.dot_general(qw[g, span, :], kk, (((1,), (1,)), ((), ())),
                                    preferred_element_type=F32)
                s = jnp.where(ok, s, -1e30)
                sink = sink_ref[0:1, g:g + 1] * LOG2E
                m = jnp.maximum(jnp.max(s, axis=-1, keepdims=True), sink)
                p = jnp.exp2(s - m)
                den = jnp.sum(p, axis=-1, keepdims=True) + jnp.exp2(sink - m)
                o = jnp.dot(p.astype(BF16), vv, preferred_element_type=F32) / den
                outs.append(o[:, kv * HEAD:(kv + 1) * HEAD])
            omw[span, :] = jnp.concatenate(outs, axis=-1).astype(BF16)
            return 0

        lax.fori_loop(0, nr, one, 0)

    half = n_sp // 2

    def ring_step(e, _):
        d, j = e // 2 + 1, e % 2
        r = 2 * j + core
        for way in range(2):
            last = half - core if way == 0 else half - 1 + core
            b = member(-d) if way == 0 else member(d)
            dev = at(s=right) if way == 0 else at(s=left)

            @pl.when((e < n_sp) & (d <= last))
            def _():
                for c in ring_copies(b, r, way, dev):
                    c.wait_recv()

                @pl.when(d < last)
                def _():
                    for c in ring_copies(b, r, way, dev):
                        c.start()

                for c in mate_copies(b, r):
                    c.start()

        d1 = e // 2
        b = jnp.where(e == 0, sp, jnp.where(j == 0, member(-d1), member(d1)))

        @pl.when(e >= 2)
        def _():
            for i in range(nr // 2):
                for c in mate_copies(b, 2 * i + 1 - core):
                    c.wait_recv()

        @pl.when(e == 1)
        def _():
            window()

        @pl.when(e != 1)
        def _():
            block(b)
        return 0

    lax.fori_loop(0, n_sp + 1, ring_step, 0)
    weights[7].wait()
    weights[8].wait()

    for i in range(heads // 2):
        def norm(h):
            a = acc[h]
            return a, pltpu.roll(a, NOPE, 1)
        a0, b0 = norm(2 * i)
        a1, b1 = norm(2 * i + 1)
        low = lax.broadcasted_iota(jnp.int32, a0.shape, 1) < NOPE
        oml[:, i * 128:(i + 1) * 128] = (
            jnp.where(low, b0, a1) / jnp.where(low, a0, b1)).astype(BF16)

    def pcopy(r, k):
        return rcopy(part_p.at[k, r], prec.at[k, r], psend.at[k, r], precv.at[k, r], at(t=mate))

    def scopy(r, dx):
        k = xpeer(dx)
        return rcopy(xs.at[dx, r], xr.at[dx, r], ssend.at[dx, r], srecv.at[dx, r],
                     at(t=k * 2 + core))

    def partial(r, t):
        span = pl.ds(pl.multiple_of(r * CH, CH), CH)
        cols = pl.ds(pl.multiple_of(t * feat, 128), feat)
        return jnp.dot(oml[span, :], ol[:, cols], preferred_element_type=F32) + jnp.dot(
            omw[span, :], ow[:, cols], preferred_element_type=F32)

    def scatter_step(e, _):
        @pl.when(e < nr)
        def _():
            for k in range(nx):
                part_p[k, e] = partial(e, 2 * k + 1 - core).astype(BF16)
                pcopy(e, k).start()
            for k in range(nx):
                part_m[k, e] = partial(e, 2 * k + core)

        @pl.when(e >= 1)
        def _():
            r = e - 1
            for k in range(nx):
                pcopy(r, k).wait_recv()
            for dx in range(1, nx):
                k = xpeer(dx)
                xs[dx, r] = (part_m[k, r] + prec[k, r].astype(F32)).astype(BF16)
                scopy(r, dx).start()
        return 0

    lax.fori_loop(0, nr + 1, scatter_step, 0)

    def final_step(r, _):
        total = part_m[xi, r] + prec[xi, r].astype(F32)
        for dx in range(1, nx):
            scopy(r, dx).wait_recv()
            total = total + xr[dx, r].astype(F32)
        out_ref[pl.ds(pl.multiple_of(r * CH, CH), CH), :] = total.astype(BF16)
        return 0

    lax.fori_loop(0, nr, final_step, 0)

    def drain_rows(r, _):
        xmate(r).wait_send()
        for dx in range(1, nx):
            xcopy(r, dx).wait_send()
            xforward(r, dx).wait_send()
            scopy(r, dx).wait_send()
        for k in range(nx):
            pcopy(r, k).wait_send()
        return 0

    lax.fori_loop(0, nr, drain_rows, 0)
    for i in range(2):
        for c in halo(i):
            c.wait_send()

    def drain_ring(e, _):
        d, j = e // 2, e % 2
        r = 2 * j + core
        for way in range(2):
            last = half - core if way == 0 else half - 1 + core
            b = member(-d) if way == 0 else member(d)
            dev = at(s=right) if way == 0 else at(s=left)

            @pl.when(d < last)
            def _():
                for c in ring_copies(b, r, way, dev):
                    c.wait_send()

            @pl.when((d >= 1) & (d <= last))
            def _():
                for c in mate_copies(b, r):
                    c.wait_send()
        return 0

    lax.fori_loop(0, n_sp + 2, drain_ring, 0)


def tables(rows, n_sp):
    freq_w = 10000.0 ** (-np.arange(32) / 32.0)
    freq_l = 10000.0 ** (-np.arange(16) / 16.0)
    freq = np.concatenate([freq_w, freq_w, freq_l, freq_l, np.zeros(32)])
    is_sin = np.concatenate(
        [np.zeros(32), np.ones(32), np.zeros(16), np.ones(16), np.zeros(32)]) > 0
    inner = np.arange(rows)[:, None] * freq[None]
    c, s = np.cos(inner), np.sin(inner)
    first = np.where(is_sin, s, c).astype(np.float32)
    second = np.where(is_sin, c, -s).astype(np.float32)
    outer = (np.arange(n_sp) * rows)[:, None] * freq[None]
    offs = np.stack([np.cos(outer), np.sin(outer)], axis=1).astype(np.float32)
    return first, second, offs


def shards(n_sp, n_tp, x, gain, lq, ld, rd, lgain, lu, wq, wk, wv, sink, ol, ow):
    rows, feat = x.shape
    nr = rows // CH
    nx = n_tp // 2
    heads = lu.shape[1] // (NOPE + HEAD)
    wheads = wq.shape[1] // HEAD
    kheads = wk.shape[1] // HEAD
    latent = ld.shape[1]
    dims = (n_sp, n_tp, rows, feat, heads, wheads, kheads)
    first, second, offs = tables(rows, n_sp)
    vm = pl.BlockSpec(memory_space=pltpu.VMEM)
    hb = pl.BlockSpec(memory_space=pl.ANY)
    rd = rd.T
    big = [lq, ld, rd, lu, wq, wk, wv, ol, ow]
    dma = pltpu.SemaphoreType.DMA
    scratch = [pltpu.VMEM(a.shape, a.dtype) for a in big] + [
        pltpu.VMEM((n_tp, nr, CH, feat), BF16),
        pltpu.VMEM((CH, n_tp * feat), BF16),
        pltpu.VMEM((n_sp, nr, CH, latent), BF16),
        pltpu.VMEM((n_sp, nr, ROPE, CH), BF16),
        pltpu.VMEM((heads, rows, 128), BF16),
        pltpu.VMEM((wheads, rows, kheads * HEAD), BF16),
        pltpu.VMEM((nr + 2, CH, kheads * HEAD), BF16),
        pltpu.VMEM((nr + 2, CH, kheads * HEAD), BF16),
        pltpu.VMEM((heads * NOPE, latent), BF16),
        pltpu.VMEM((heads, 128, rows), BF16),
        pltpu.VMEM((heads, rows, 128), BF16),
        pltpu.VMEM((heads, rows, 128), F32),
        pltpu.VMEM((heads, rows, 128), F32),
        pltpu.VMEM((rows, heads * HEAD), BF16),
        pltpu.VMEM((rows, wheads * HEAD), BF16),
        pltpu.VMEM((nx, nr, CH, feat), BF16),
        pltpu.VMEM((nx, nr, CH, feat), F32),
        pltpu.VMEM((nx, nr, CH, feat), BF16),
        pltpu.VMEM((nx, nr, CH, feat), BF16),
        pltpu.VMEM((nx, nr, CH, feat), BF16),
        dma((9,)),
        dma((nx, nr)), dma((n_tp, nr)), dma((nx, nr)),
        dma((2, n_sp, 2)), dma((n_sp, nr)), dma((n_sp, 2)),
        dma((2, n_sp, 2)), dma((n_sp, nr)), dma((n_sp, 2)),
        dma((2, 2)), dma((2, 2)),
        dma((nx, nr)), dma((nx, nr)), dma((nx, nr)), dma((nx, nr)),
    ]
    return pl.pallas_call(
        functools.partial(body, dims),
        out_shape=jax.ShapeDtypeStruct((rows, feat), BF16),
        in_specs=[vm, vm, hb, hb, hb, vm, hb, hb, hb, hb, vm, hb, hb, vm, vm, vm],
        out_specs=vm,
        scratch_shapes=scratch,
        compiler_params=pltpu.CompilerParams(
            collective_id=0, has_side_effects=True, vmem_limit_bytes=60 * 1024 * 1024),
    )(x, gain[None], lq, ld, rd, lgain[None], lu, wq, wk, wv, sink[None], ol, ow,
      jnp.asarray(first), jnp.asarray(second), jnp.asarray(offs))


def solution(mesh):
    in_specs = (
        P("sp", "tp"),
        P(),
        P(None, "tp"),
        P(),
        P(),
        P(),
        P(None, "tp"),
        P(None, "tp"),
        P(None, "tp"),
        P(None, "tp"),
        P("tp"),
        P("tp", None),
        P("tp", None),
    )
    step = functools.partial(shards, mesh.shape["sp"], mesh.shape["tp"])
    return jax.shard_map(
        step, mesh=mesh, in_specs=in_specs, out_specs=P("sp", "tp"), check_vma=False)
```
